32 devices in a mesh: ep: 8 (over z, y), tp: 4 (over x, core).
Axes of the slice: x: 2, y: 2, z: 4, core: 2. Of those that a mesh axis runs over, the one named last changes fastest.
Arguments:
- tokens: bfloat16 [256, 2048], P('ep'), may hold values from -6 to 6
- in_gain: float32 [2048], replicated, may hold values from 0.1 to 1.9
- expert_ids: int32 [256, 2], P('ep'), may hold values from 0 to 7, all different within a row; in each aligned block of 32 rows (0 to 31, 32 to 63, ...) at most 16 rows name the same one
- route_weight: float32 [256, 2], P('ep'), may hold values from 0.1 to 1
- w_gate: bfloat16 [8, 2048, 1024], P('ep', None, 'tp'), may hold values from -0.125 to 0.125
- w_up: bfloat16 [8, 2048, 1024], P('ep', None, 'tp'), may hold values from -0.125 to 0.125
- w_down: bfloat16 [8, 1024, 2048], P('ep', 'tp'), may hold values from -0.1875 to 0.1875
- out_gain: float32 [2048], P('tp'), may hold values from 0.1 to 1.9
Outputs:
- mixed: bfloat16 [256, 2048], P('ep', 'tp')
The draws below stay inside these ranges and needn't reach their ends.
Inputs may be any that keep to these rules, and one draw needn't show every extreme that they name: `expert_ids`: each token names 2 different experts; among the tokens of one index of ep no expert is named more than 16 times, and in every draw the tokens of some index of ep name some expert exactly 16 times; every expert is named by some token.
All inputs are finite; a program needn't handle non-finite values.
Results may differ from the reference program's by a relative error of at most 0.002.
Values may be sent and summed in bfloat16 or wider, within the bound.
A program may use at most 64 MiB of HBM per device.

```python
import math
import jax
import jax.numpy as jnp
import numpy as np
from jax import lax

D = 2048
FF = 1024
TOPK = 2
TOK_DEV = 32
TOKENS = 256
EXPERTS = 8
CAP = 16


def level_of(key, extent, pieces, least, largest):
    loudness, own = 1.0, jax.random.fold_in(key, 6)
    for axis_at, shards_of in pieces:
        heights = jnp.exp(jax.random.uniform(jax.random.fold_in(own, axis_at), (shards_of,), jnp.float32, least / len(pieces), largest / len(pieces)))
        loudness = loudness * jnp.repeat(heights, extent[axis_at] // shards_of).reshape([-1 if axis == axis_at else 1 for axis in range(len(extent))])
    return loudness


def routed_block(rng, own, number, rows, amount, top, limit, skew):
    order = jax.random.permutation(rng, amount)
    packed, ordinary = portions_of(amount, rows * top, limit, skew, True), portions_of(amount, rows * top, limit, skew, False)
    places = jnp.arange(amount)

    def named(sizes, offset_by):
        used = int((sizes > 0).sum())
        fixed = max(1, used // 4)
        moved = fixed + (places - fixed + offset_by * (used - fixed)) % max(1, amount - fixed)
        return jnp.zeros((amount,), jnp.int32).at[order[jnp.where(places < fixed, places, moved)]].set(jnp.asarray(sizes, jnp.int32))

    sizes = jnp.where(number % 4 == 0, named(packed, number // 4), named(ordinary, number - number // 4 - 1))
    mixed = jax.random.permutation(jax.random.fold_in(own, 3), amount)
    donor, receiver = mixed[0:amount // 2 * 2:2], mixed[1:amount // 2 * 2:2]
    room = jnp.minimum(sizes[donor] - 1, limit - sizes[receiver]) // 2
    room = jnp.where((donor == order[0]) | (receiver == order[0]) | (sizes[receiver] == 0), 0, jnp.maximum(room, 0))
    moved = jax.random.randint(jax.random.fold_in(own, 4), (amount // 2,), 0, 1 << 20) % (room + 1)
    sizes = sizes.at[donor].add(-moved).at[receiver].add(moved)
    members = jnp.searchsorted(jnp.cumsum(sizes), jnp.arange(rows * top), side="right").astype(jnp.int32)
    grid = members.reshape(top, rows).T
    grid = grid[jax.random.permutation(jax.random.fold_in(own, 1), rows)]
    offset_by = jax.random.randint(jax.random.fold_in(own, 2), (rows, 1), 0, top)
    return jnp.take_along_axis(grid, (jnp.arange(top)[None, :] + offset_by) % top, axis=1)


def portions_of(number_of, total, most, skew, full):
    portions = [(1 << 20) // math.isqrt(grade ** skew) + 1 for grade in range(1, number_of + 1)]
    largest = most if full else min(most, max(-(-total // number_of), total * portions[0] // sum(portions)))
    least = 1 if total - largest >= number_of - 1 else 0
    holding, surplus = [largest] + [least] * (number_of - 1), total - largest - least * (number_of - 1)
    while surplus > 0:
        movable = [i for i in range(1, number_of) if holding[i] < largest] or [i for i in range(1, number_of) if holding[i] < most]
        mass, left = sum([portions[i] for i in movable]), surplus
        for i in movable:
            addition = min(most - holding[i], max(1, left * portions[i] // mass), surplus)
            holding[i] = holding[i] + addition
            surplus = surplus - addition
    return np.array(holding)


def gaussian(key, dims, deviation, bound, cuts=(), kind=jnp.bfloat16):
    array = deviation * jax.random.normal(key, dims, jnp.float32)
    if cuts:
        array = array * level_of(key, dims, cuts, -0.22, 0.18)
    return jnp.clip(array, -bound, bound).astype(kind)


def setup_inputs(seed: int = 0) -> dict:
    key_list = jax.random.split(jax.random.key(seed), 9)
    tokens = gaussian(key_list[0], (TOKENS, D), 1.0, 6.0, ((0, 8),))
    in_gain = jnp.clip(1.0 + 0.18 * jax.random.normal(key_list[1], (D,), jnp.float32), 0.1, 1.9)
    expert_ids_keys = jax.random.split(jax.random.fold_in(key_list[2], 1), TOKENS // TOK_DEV)
    expert_ids_turns = jax.random.permutation(jax.random.fold_in(key_list[2], 3), TOKENS // TOK_DEV)
    expert_ids = jax.vmap(lambda own, number: routed_block(jax.random.fold_in(key_list[2], 2), own, number, TOK_DEV, EXPERTS, TOPK, CAP, 2))(expert_ids_keys, expert_ids_turns).reshape((TOKENS, TOPK))
    route_weight = jnp.clip(0.1 + 0.9 * jax.random.uniform(key_list[3], (TOKENS, TOPK), jnp.float32) ** level_of(key_list[3], (TOKENS, TOPK), ((0, 8),), -0.2, 0.2), 0.1, 1.0)
    w_gate = gaussian(key_list[4], (EXPERTS, D, FF), D ** -0.5, 0.125, ((0, 8), (2, 4)))
    w_up = gaussian(key_list[5], (EXPERTS, D, FF), D ** -0.5, 0.125, ((0, 8), (2, 4)))
    w_down = gaussian(key_list[6], (EXPERTS, FF, D), FF ** -0.5, 0.1875, ((0, 8), (1, 4)))
    out_gain = jnp.clip(1.0 + 0.18 * jax.random.normal(key_list[7], (D,), jnp.float32), 0.1, 1.9)
    return dict(tokens=tokens, in_gain=in_gain, expert_ids=expert_ids, route_weight=route_weight, w_gate=w_gate, w_up=w_up, w_down=w_down, out_gain=out_gain)


norm_eps = 1e-05
block_rows = 128

def norm_rows(values, gain):
    centre = lax.optimization_barrier(jnp.mean(values, axis=-1, keepdims=True))
    centered = values - centre
    spread = lax.optimization_barrier(jnp.mean(centered * centered, axis=-1, keepdims=True))
    return centered * lax.rsqrt(spread + norm_eps) * gain

def reference(tokens, in_gain, expert_ids, route_weight, w_gate, w_up, w_down, out_gain):
    normed = norm_rows(tokens.astype(jnp.float32), in_gain).astype(jnp.bfloat16)
    routes_flat = expert_ids.reshape(-1).astype(jnp.int32)
    total = routes_flat.shape[0]
    experts = w_gate.shape[0]
    order = jnp.argsort(routes_flat, stable=True).astype(jnp.int32)
    counts = jnp.zeros((experts,), jnp.int32).at[routes_flat].add(1)
    blocks = (counts + block_rows - 1) // block_rows
    block_start = (jnp.cumsum(blocks) - blocks).astype(jnp.int32)
    row_start = (jnp.cumsum(counts) - counts).astype(jnp.int32)
    sorted_ids = routes_flat[order]
    rank_sorted = jnp.arange(total, dtype=jnp.int32) - row_start[sorted_ids]
    pos_sorted = block_start[sorted_ids] * block_rows + rank_sorted
    positions = jnp.zeros((total,), jnp.int32).at[order].set(pos_sorted.astype(jnp.int32))
    block_count = total // block_rows + 1 + experts
    token_of = jnp.arange(total, dtype=jnp.int32) // TOPK
    buffer = jnp.zeros((block_count * block_rows, normed.shape[1]), normed.dtype)
    buffer = buffer.at[positions].set(normed[token_of])
    owners = (jnp.searchsorted(block_start, jnp.arange(block_count, dtype=jnp.int32), side='right') - 1).astype(jnp.int32)

    def one_block(operands):
        block_in, owner = operands
        gate_w = lax.dynamic_index_in_dim(w_gate, owner, 0, keepdims=False)
        up_w = lax.dynamic_index_in_dim(w_up, owner, 0, keepdims=False)
        down_w = lax.dynamic_index_in_dim(w_down, owner, 0, keepdims=False)
        gate_act = jnp.dot(block_in, gate_w, preferred_element_type=jnp.float32)
        up_act = jnp.dot(block_in, up_w, preferred_element_type=jnp.float32)
        hidden = (jax.nn.silu(gate_act) * up_act).astype(block_in.dtype)
        return jnp.dot(hidden, down_w, preferred_element_type=jnp.float32)
    outputs = lax.map(one_block, (buffer.reshape(block_count, block_rows, -1), owners))
    picked = outputs.reshape(block_count * block_rows, -1)[positions]
    weighted = picked * route_weight.reshape(-1, 1).astype(jnp.float32)
    mixture = lax.optimization_barrier(jnp.sum(weighted.reshape(tokens.shape[0], TOPK, -1), axis=1))
    return norm_rows(mixture, out_gain).astype(jnp.bfloat16)
```

```python
import functools

import jax
import jax.numpy as jnp
from jax import lax
from jax.experimental import pallas as pl
from jax.experimental.pallas import tpu as pltpu
from jax.sharding import PartitionSpec as P

norm_eps = 1e-05
MESH = pl.DeviceIdType.MESH


def capacity_of(tok_rows, top_count, local_experts, experts):
    return max(
        2, min(tok_rows // (2 * local_experts), (5 * tok_rows * top_count + experts - 1) // experts)
    )


def fused(
    groups, parts, inner, cap,
    tokens, in_gain, ids, weights, w_gate, w_up, w_down, out_gain,
    out,
    gate_v, up_v, down_v, sent, arrived, part, half_in, half, quarter_in, reduced, returned, stats,
    w_sem, ep_send, ep_recv, tp_send, tp_recv, in_send, in_recv, out_send, out_recv,
    ret_send, ret_recv, st_send, st_recv,
):
    outer = parts // inner
    ep, tp = lax.axis_index("ep"), lax.axis_index("tp")
    o, i = tp // inner, tp % inner
    tok, width = tokens.shape
    slots = groups * cap
    piece = width // parts

    def rows(g):
        return pl.ds(pl.multiple_of(g * cap, cap), cap)

    def cols(b):
        return pl.ds(pl.multiple_of(b * piece, piece), piece)

    barrier = pltpu.get_barrier_semaphore()
    for off in range(1, groups):
        pl.semaphore_signal(barrier, inc=1, device_id=((ep + off) % groups, tp), device_id_type=MESH)
    for j in range(1, parts):
        pl.semaphore_signal(barrier, inc=1, device_id=(ep, (tp + j) % parts), device_id_type=MESH)

    loads = [
        pltpu.make_async_copy(src.at[0], dst, w_sem.at[n])
        for n, (src, dst) in enumerate(((w_gate, gate_v), (w_up, up_v), (w_down, down_v)))
    ]
    for load in loads:
        load.start()

    values = tokens[...].astype(jnp.float32)
    centred = values - jnp.mean(values, axis=1, keepdims=True)
    spread = jnp.mean(centred * centred, axis=1, keepdims=True)
    normed = (centred * lax.rsqrt(spread + norm_eps) * in_gain[...]).astype(jnp.bfloat16)

    lane = lax.broadcasted_iota(jnp.int32, (tok, slots), 1)
    owner = jnp.zeros((tok, slots), jnp.int32)
    for g in range(1, groups):
        owner = owner + jnp.where(lane >= g * cap, 1, 0)
    slot = (lane - owner * cap).astype(jnp.float32)
    named = jnp.zeros((tok, slots), jnp.float32)
    scale = jnp.zeros((tok, slots), jnp.float32)
    for k in range(ids.shape[1]):
        hit = ids[:, k:k + 1] == owner
        named = named + jnp.where(hit, 1.0, 0.0)
        scale = scale + jnp.where(hit, weights[:, k:k + 1], 0.0)
    earlier = (
        lax.broadcasted_iota(jnp.int32, (tok, tok), 1) < lax.broadcasted_iota(jnp.int32, (tok, tok), 0)
    )
    before = jnp.dot(
        jnp.where(earlier, 1.0, 0.0).astype(jnp.bfloat16), named.astype(jnp.bfloat16),
        preferred_element_type=jnp.float32,
    )
    chosen = jnp.where(before == slot, named, 0.0)
    scale = chosen * scale
    picked = chosen.T.astype(jnp.bfloat16)
    sent[...] = jnp.dot(picked, normed, preferred_element_type=jnp.float32).astype(jnp.bfloat16)

    pl.semaphore_wait(barrier, groups - 1 + parts - 1)

    order = sorted(range(1, groups), key=lambda off: -min(off, groups - off))
    scatter = {}
    for off in order:
        to = (ep + off) % groups
        scatter[off] = pltpu.make_async_remote_copy(
            src_ref=sent.at[rows(to), cols(tp)], dst_ref=arrived.at[rows(ep), cols(tp)],
            send_sem=ep_send.at[off], recv_sem=ep_recv.at[off],
            device_id=(to, tp), device_id_type=MESH,
        )
        scatter[off].start()
    arrived[rows(ep), :] = sent[rows(ep), :]
    spread_out = []
    for off in order[::-1]:
        came = (ep + groups - off) % groups
        scatter[off].wait_recv()
        for j in range(1, parts):
            copy = pltpu.make_async_remote_copy(
                src_ref=arrived.at[rows(came), cols(tp)], dst_ref=arrived.at[rows(came), cols(tp)],
                send_sem=tp_send.at[off, j], recv_sem=tp_recv.at[off, j],
                device_id=(ep, (tp + j) % parts), device_id_type=MESH,
            )
            copy.start()
            spread_out.append(copy)
    for load in loads:
        load.wait()
    for copy in spread_out:
        copy.wait_recv()

    inputs = arrived[...]
    gate_act = jnp.dot(inputs, gate_v[...], preferred_element_type=jnp.float32)
    up_act = jnp.dot(inputs, up_v[...], preferred_element_type=jnp.float32)
    hidden = (gate_act / (1.0 + jnp.exp(-gate_act)) * up_act).astype(jnp.bfloat16)

    def down(b):
        return jnp.dot(hidden, down_v[:, cols(b)], preferred_element_type=jnp.float32)

    far = [(o + j) % outer for j in range(1, outer)]
    places = far + [o]
    inner_copies = []
    for n in range(1, inner):
        other = (i + n) % inner
        for p, place in enumerate(places):
            part[n - 1, p] = down(place * inner + other)
            copy = pltpu.make_async_remote_copy(
                src_ref=part.at[n - 1, p], dst_ref=half_in.at[n - 1, p],
                send_sem=in_send.at[n - 1, p], recv_sem=in_recv.at[n - 1, p],
                device_id=(ep, o * inner + other), device_id_type=MESH,
            )
            copy.start()
            inner_copies.append(copy)
    for p, place in enumerate(places):
        half[p] = down(place * inner + i)

    targets = order + [0]
    outer_copies = {}
    for p in range(outer - 1):
        for n in range(1, inner):
            inner_copies[(n - 1) * outer + p].wait_recv()
        for off in targets:
            at = rows((ep + off) % groups)
            total = half[p, at]
            for n in range(1, inner):
                total = total + half_in[n - 1, p, at]
            half[p, at] = total
            copy = pltpu.make_async_remote_copy(
                src_ref=half.at[p, at], dst_ref=quarter_in.at[p, at],
                send_sem=out_send.at[p, off], recv_sem=out_recv.at[p, off],
                device_id=(ep, far[p] * inner + i), device_id_type=MESH,
            )
            copy.start()
            outer_copies[p, off] = copy
    for n in range(1, inner):
        inner_copies[(n - 1) * outer + outer - 1].wait_recv()
    back = {}
    for off in targets:
        to = (ep + off) % groups
        at = rows(to)
        total = half[outer - 1, at]
        for n in range(1, inner):
            total = total + half_in[n - 1, outer - 1, at]
        for p in range(outer - 1):
            outer_copies[p, off].wait_recv()
            total = total + quarter_in[p, at]
        if off == 0:
            returned[at] = total
        else:
            reduced[at] = total
            back[off] = pltpu.make_async_remote_copy(
                src_ref=reduced.at[at], dst_ref=returned.at[rows(ep)],
                send_sem=ret_send.at[off], recv_sem=ret_recv.at[off],
                device_id=(to, tp), device_id_type=MESH,
            )
            back[off].start()
    for off in order:
        back[off].wait_recv()

    mixture = jnp.dot(
        scale, returned[...], precision=lax.Precision.HIGHEST, preferred_element_type=jnp.float32
    )
    own_mean = jnp.mean(mixture, axis=1, keepdims=True)
    own_gap = mixture - own_mean
    own_spread = jnp.sum(own_gap * own_gap, axis=1, keepdims=True)
    column = lax.broadcasted_iota(jnp.int32, (tok, 128), 1)
    stats[0] = jnp.where(column == 0, own_mean, own_spread)
    moments = []
    for j in range(1, parts):
        copy = pltpu.make_async_remote_copy(
            src_ref=stats.at[0], dst_ref=stats.at[j],
            send_sem=st_send.at[j], recv_sem=st_recv.at[j],
            device_id=(ep, (tp + j) % parts), device_id_type=MESH,
        )
        copy.start()
        moments.append(copy)
    for copy in moments:
        copy.wait_recv()
    means = [own_mean] + [stats[j][:, 0:1] for j in range(1, parts)]
    spreads = [own_spread] + [stats[j][:, 1:2] for j in range(1, parts)]
    row_mean = sum(means) / parts
    total = sum(spreads)
    for mean in means:
        total = total + piece * (mean - row_mean) * (mean - row_mean)
    out[...] = (
        (mixture - row_mean) * lax.rsqrt(total / width + norm_eps) * out_gain[...]
    ).astype(out.dtype)

    for off in order:
        scatter[off].wait_send()
        back[off].wait_send()
    for copy in spread_out + inner_copies + list(outer_copies.values()) + moments:
        copy.wait_send()


def one_kernel(groups, parts, cap, tokens, in_gain, ids, weights, w_gate, w_up, w_down, out_gain):
    inner = 2
    outer = parts // inner
    tok, width = tokens.shape
    slots, piece, hidden = groups * cap, width // parts, w_gate.shape[2]
    vmem, hbm, dma = pl.BlockSpec(memory_space=pltpu.VMEM), pl.BlockSpec(memory_space=pl.ANY), pltpu.SemaphoreType.DMA
    return pl.pallas_call(
        functools.partial(fused, groups, parts, inner, cap),
        name="experts",
        out_shape=jax.ShapeDtypeStruct((tok, piece), jnp.bfloat16),
        in_specs=[vmem, vmem, vmem, vmem, hbm, hbm, hbm, vmem],
        out_specs=vmem,
        scratch_shapes=[
            pltpu.VMEM((width, hidden), jnp.bfloat16),
            pltpu.VMEM((width, hidden), jnp.bfloat16),
            pltpu.VMEM((hidden, width), jnp.bfloat16),
            pltpu.VMEM((slots, width), jnp.bfloat16),
            pltpu.VMEM((slots, width), jnp.bfloat16),
            pltpu.VMEM((inner - 1, outer, slots, piece), jnp.float32),
            pltpu.VMEM((inner - 1, outer, slots, piece), jnp.float32),
            pltpu.VMEM((outer, slots, piece), jnp.float32),
            pltpu.VMEM((outer, slots, piece), jnp.float32),
            pltpu.VMEM((slots, piece), jnp.float32),
            pltpu.VMEM((slots, piece), jnp.float32),
            pltpu.VMEM((parts, tok, 128), jnp.float32),
            dma((3,)), dma((groups,)), dma((groups,)), dma((groups, parts)), dma((groups, parts)),
            dma((inner - 1, outer)), dma((inner - 1, outer)), dma((outer, groups)), dma((outer, groups)),
            dma((groups,)), dma((groups,)), dma((parts,)), dma((parts,)),
        ],
        compiler_params=pltpu.CompilerParams(collective_id=0, has_side_effects=True),
    )(tokens, in_gain.reshape(1, -1), ids, weights, w_gate, w_up, w_down, out_gain.reshape(1, -1))


def collectives(tokens, in_gain, expert_ids, route_weight, w_gate, w_up, w_down, out_gain):
    tok_rows = tokens.shape[0]
    top_count = expert_ids.shape[1]
    local_experts = w_gate.shape[0]
    groups = lax.axis_size("ep")
    experts = local_experts * groups
    capacity = capacity_of(tok_rows, top_count, local_experts, experts)
    values = tokens.astype(jnp.float32)
    row_centre = jnp.mean(values, axis=1, keepdims=True)
    centered_in = values - row_centre
    spread_in = jnp.mean(centered_in * centered_in, axis=1, keepdims=True)
    normed = (centered_in * lax.rsqrt(spread_in + norm_eps) * in_gain).astype(jnp.bfloat16)
    routes_flat = expert_ids.reshape(-1)
    labels = lax.broadcasted_iota(jnp.int32, (1, experts), 1)
    one_hot = (routes_flat[:, None] == labels).astype(jnp.int32)
    before = jnp.cumsum(one_hot, axis=0) - one_hot
    slot_index = jnp.sum(before * one_hot, axis=1)
    positions = routes_flat * capacity + slot_index
    source = jnp.repeat(normed, top_count, axis=0)
    outgoing = (
        jnp.zeros((experts * capacity, normed.shape[1]), jnp.bfloat16).at[positions].set(source)
    )
    arrived = lax.all_to_all(outgoing, "ep", split_axis=0, concat_axis=0, tiled=True)
    arrived = arrived.reshape(groups, local_experts, capacity, normed.shape[1])
    gate_act = jnp.einsum("sjcd,jdf->sjcf", arrived, w_gate, preferred_element_type=jnp.float32)
    up_act = jnp.einsum("sjcd,jdf->sjcf", arrived, w_up, preferred_element_type=jnp.float32)
    hidden = (jax.nn.silu(gate_act) * up_act).astype(jnp.bfloat16)
    partial_value = jnp.einsum("sjcf,jfd->sjcd", hidden, w_down, preferred_element_type=jnp.float32)
    partial_value = partial_value.reshape(experts * capacity, normed.shape[1])
    weights = route_weight.reshape(-1, 1)

    def combine(returned):
        picked = returned[positions] * weights
        return jnp.sum(picked.reshape(tok_rows, top_count, -1), axis=1)

    summed = lax.psum_scatter(partial_value, "tp", scatter_dimension=1, tiled=True)
    returned = lax.all_to_all(summed, "ep", split_axis=0, concat_axis=0, tiled=True)
    mixture = combine(returned)
    full_width = mixture.shape[1] * lax.axis_size("tp")
    row_total = lax.psum(jnp.sum(mixture, axis=1, keepdims=True), "tp")
    row_mean = row_total / full_width
    centered = mixture - row_mean
    deviations = lax.psum(jnp.sum(centered * centered, axis=1, keepdims=True), "tp")
    spread = deviations / full_width
    return (centered * lax.rsqrt(spread + norm_eps) * out_gain).astype(jnp.bfloat16)


def shards(tokens, in_gain, expert_ids, route_weight, w_gate, w_up, w_down, out_gain):
    groups, parts = lax.axis_size("ep"), lax.axis_size("tp")
    tok_rows, width = tokens.shape
    local_experts = w_gate.shape[0]
    cap = capacity_of(tok_rows, expert_ids.shape[1], local_experts, local_experts * groups)
    whole_tiles = cap % 16 == 0 and (groups * cap) % 128 == 0 and width % (parts * 128) == 0
    if local_experts == 1 and parts % 2 == 0 and whole_tiles and groups * cap * width <= 1 << 20:
        return one_kernel(
            groups, parts, cap, tokens, in_gain, expert_ids, route_weight, w_gate, w_up, w_down, out_gain
        )
    return collectives(
        tokens, in_gain, expert_ids, route_weight, w_gate, w_up, w_down, out_gain
    )


def solution(mesh):
    in_specs = (
        P("ep", None),
        P(),
        P("ep", None),
        P("ep", None),
        P("ep", None, "tp"),
        P("ep", None, "tp"),
        P("ep", "tp", None),
        P("tp"),
    )
    out_specs = P("ep", "tp")
    return jax.shard_map(shards, mesh=mesh, in_specs=in_specs, out_specs=out_specs, check_vma=False)
```

```python
import functools

import jax
import jax.numpy as jnp
from jax import lax
from jax.experimental import pallas as pl
from jax.experimental.pallas import tpu as pltpu
from jax.sharding import PartitionSpec as P

norm_eps = 1e-05
MESH = pl.DeviceIdType.MESH


def capacity_of(tok_rows, top_count, local_experts, experts):
    return max(
        2, min(tok_rows // (2 * local_experts), (5 * tok_rows * top_count + experts - 1) // experts)
    )


def fused(
    groups, parts, inner, cap,
    tokens_h, in_gain_h, ids_h, weights_h, w_gate, w_up, w_down, out_gain_h,
    out_h,
    tokens, in_gain, ids, weights, out_gain, out, picked, row_sem,
    gate_v, up_v, down_v, sent, arrived, part, half_in, half, quarter_in, reduced, returned, stats,
    w_sem, ep_send, ep_recv, tp_send, tp_recv, in_send, in_recv, out_send, out_recv,
    ret_send, ret_recv, st_send, st_recv,
):
    outer = parts // inner
    ep, tp = lax.axis_index("ep"), lax.axis_index("tp")
    o, i = tp // inner, tp % inner
    tok, width = tokens.shape
    slots = groups * cap
    piece = width // parts

    def rows(g):
        return pl.ds(pl.multiple_of(g * cap, cap), cap)

    def cols(b):
        return pl.ds(pl.multiple_of(b * piece, piece), piece)

    barrier = pltpu.get_barrier_semaphore()
    for off in range(1, groups):
        pl.semaphore_signal(barrier, inc=1, device_id=((ep + off) % groups, tp), device_id_type=MESH)
    for j in range(1, parts):
        pl.semaphore_signal(barrier, inc=1, device_id=(ep, (tp + j) % parts), device_id_type=MESH)

    row_loads = [
        pltpu.make_async_copy(src, dst, row_sem.at[n])
        for n, (src, dst) in enumerate((
            (tokens_h, tokens), (in_gain_h, in_gain), (ids_h, ids), (weights_h, weights),
            (out_gain_h, out_gain),
        ))
    ]
    for load in row_loads:
        load.start()
    loads = [
        pltpu.make_async_copy(src.at[0], dst, w_sem.at[n])
        for n, (src, dst) in enumerate(((w_gate, gate_v), (w_up, up_v), (w_down, down_v)))
    ]
    for load in loads:
        load.start()

    for load in row_loads:
        load.wait()
    values = tokens[...].astype(jnp.float32)
    centred = values - jnp.mean(values, axis=1, keepdims=True)
    spread = jnp.mean(centred * centred, axis=1, keepdims=True)
    normed = (centred * lax.rsqrt(spread + norm_eps) * in_gain[...]).astype(jnp.bfloat16)

    lane = lax.broadcasted_iota(jnp.int32, (slots, tok), 0)
    owner = jnp.zeros((slots, tok), jnp.int32)
    for g in range(1, groups):
        owner = owner + jnp.where(lane >= g * cap, 1, 0)
    slot = (lane - owner * cap).astype(jnp.float32)
    named = jnp.zeros((slots, tok), jnp.float32)
    scale = jnp.zeros((slots, tok), jnp.float32)
    for k in range(ids.shape[0]):
        hit = ids[k:k + 1, :] == owner
        named = named + jnp.where(hit, 1.0, 0.0)
        scale = scale + jnp.where(hit, weights[k:k + 1, :], 0.0)
    earlier = (
        lax.broadcasted_iota(jnp.int32, (tok, tok), 0) < lax.broadcasted_iota(jnp.int32, (tok, tok), 1)
    )
    before = jnp.dot(
        named.astype(jnp.bfloat16), jnp.where(earlier, 1.0, 0.0).astype(jnp.bfloat16),
        preferred_element_type=jnp.float32,
    )
    chosen = jnp.where(before == slot, named, 0.0)
    picked[...] = chosen * scale
    sent[...] = jnp.dot(
        chosen.astype(jnp.bfloat16), normed, preferred_element_type=jnp.float32
    ).astype(jnp.bfloat16)

    pl.semaphore_wait(barrier, groups - 1 + parts - 1)

    order = sorted(range(1, groups), key=lambda off: -min(off, groups - off))
    scatter = {}
    for off in order:
        to = (ep + off) % groups
        scatter[off] = pltpu.make_async_remote_copy(
            src_ref=sent.at[rows(to), cols(tp)], dst_ref=arrived.at[rows(ep), cols(tp)],
            send_sem=ep_send.at[off], recv_sem=ep_recv.at[off],
            device_id=(to, tp), device_id_type=MESH,
        )
        scatter[off].start()
    arrived[rows(ep), :] = sent[rows(ep), :]
    spread_out, relays, local = [], {}, []

    def share(off, block, j, to):
        came = (ep + groups - off) % groups
        copy = pltpu.make_async_remote_copy(
            src_ref=arrived.at[rows(came), cols(block)], dst_ref=arrived.at[rows(came), cols(block)],
            send_sem=tp_send.at[off, j], recv_sem=tp_recv.at[off, j],
            device_id=(ep, to), device_id_type=MESH,
        )
        copy.start()
        spread_out.append(copy)
        return copy

    for off in order[::-1]:
        scatter[off].wait_recv()
        for a in range(1, outer):
            relays[off, a] = share(off, tp, a * inner, (o + a) % outer * inner + i)
        for b in range(1, inner):
            local.append(share(off, tp, b, o * inner + (i + b) % inner))
    for off in order[::-1]:
        for a in range(1, outer):
            relays[off, a].wait_recv()
            block = (o + outer - a) % outer * inner + i
            for b in range(1, inner):
                local.append(share(off, block, a * inner + b, o * inner + (i + b) % inner))
    for load in loads:
        load.wait()
    for copy in local:
        copy.wait_recv()

    inputs = arrived[...]
    gate_act = jnp.dot(inputs, gate_v[...], preferred_element_type=jnp.float32)
    up_act = jnp.dot(inputs, up_v[...], preferred_element_type=jnp.float32)
    hidden = (gate_act / (1.0 + jnp.exp(-gate_act)) * up_act).astype(jnp.bfloat16)

    def down(b):
        return jnp.dot(hidden, down_v[:, cols(b)], preferred_element_type=jnp.float32)

    far = [(o + j) % outer for j in range(1, outer)]
    places = far + [o]
    inner_copies = []
    for n in range(1, inner):
        other = (i + n) % inner
        for p, place in enumerate(places):
            part[n - 1, p] = down(place * inner + other)
            copy = pltpu.make_async_remote_copy(
                src_ref=part.at[n - 1, p], dst_ref=half_in.at[n - 1, p],
                send_sem=in_send.at[n - 1, p], recv_sem=in_recv.at[n - 1, p],
                device_id=(ep, o * inner + other), device_id_type=MESH,
            )
            copy.start()
            inner_copies.append(copy)
    for p, place in enumerate(places):
        half[p] = down(place * inner + i)

    targets = order + [0]
    outer_copies = {}
    for p in range(outer - 1):
        for n in range(1, inner):
            inner_copies[(n - 1) * outer + p].wait_recv()
        for off in targets:
            at = rows((ep + off) % groups)
            total = half[p, at]
            for n in range(1, inner):
                total = total + half_in[n - 1, p, at]
            half[p, at] = total
            copy = pltpu.make_async_remote_copy(
                src_ref=half.at[p, at], dst_ref=quarter_in.at[p, at],
                send_sem=out_send.at[p, off], recv_sem=out_recv.at[p, off],
                device_id=(ep, far[p] * inner + i), device_id_type=MESH,
            )
            copy.start()
            outer_copies[p, off] = copy
    for n in range(1, inner):
        inner_copies[(n - 1) * outer + outer - 1].wait_recv()
    back = {}
    for off in targets:
        to = (ep + off) % groups
        at = rows(to)
        total = half[outer - 1, at]
        for n in range(1, inner):
            total = total + half_in[n - 1, outer - 1, at]
        for p in range(outer - 1):
            outer_copies[p, off].wait_recv()
            total = total + quarter_in[p, at]
        if off == 0:
            returned[at] = total
        else:
            reduced[at] = total
            back[off] = pltpu.make_async_remote_copy(
                src_ref=reduced.at[at], dst_ref=returned.at[rows(ep)],
                send_sem=ret_send.at[off], recv_sem=ret_recv.at[off],
                device_id=(to, tp), device_id_type=MESH,
            )
            back[off].start()
    for off in order:
        back[off].wait_recv()

    mixture = jnp.dot(
        picked[...].T, returned[...], precision=lax.Precision.HIGHEST, preferred_element_type=jnp.float32
    )
    own_mean = jnp.mean(mixture, axis=1, keepdims=True)
    own_gap = mixture - own_mean
    own_spread = jnp.sum(own_gap * own_gap, axis=1, keepdims=True)
    column = lax.broadcasted_iota(jnp.int32, (tok, 128), 1)
    stats[0] = jnp.where(column == 0, own_mean, own_spread)
    moments = []
    for j in range(1, parts):
        copy = pltpu.make_async_remote_copy(
            src_ref=stats.at[0], dst_ref=stats.at[j],
            send_sem=st_send.at[j], recv_sem=st_recv.at[j],
            device_id=(ep, (tp + j) % parts), device_id_type=MESH,
        )
        copy.start()
        moments.append(copy)
    for copy in moments:
        copy.wait_recv()
    means = [own_mean] + [stats[j][:, 0:1] for j in range(1, parts)]
    spreads = [own_spread] + [stats[j][:, 1:2] for j in range(1, parts)]
    row_mean = sum(means) / parts
    total = sum(spreads)
    for mean in means:
        total = total + piece * (mean - row_mean) * (mean - row_mean)
    out[...] = (
        (mixture - row_mean) * lax.rsqrt(total / width + norm_eps) * out_gain[...]
    ).astype(out.dtype)
    result = pltpu.make_async_copy(out, out_h, row_sem.at[0])
    result.start()

    for off in order:
        scatter[off].wait_send()
        back[off].wait_send()
    for copy in spread_out + inner_copies + list(outer_copies.values()) + moments:
        copy.wait_send()
    result.wait()


def one_kernel(groups, parts, cap, tokens, in_gain, ids, weights, w_gate, w_up, w_down, out_gain):
    inner = 2
    outer = parts // inner
    tok, width = tokens.shape
    slots, piece, hidden = groups * cap, width // parts, w_gate.shape[2]
    hbm, dma = pl.BlockSpec(memory_space=pl.ANY), pltpu.SemaphoreType.DMA
    return pl.pallas_call(
        functools.partial(fused, groups, parts, inner, cap),
        name="experts",
        out_shape=jax.ShapeDtypeStruct((tok, piece), jnp.bfloat16),
        in_specs=[hbm] * 8,
        out_specs=hbm,
        scratch_shapes=[
            pltpu.VMEM((tok, width), jnp.bfloat16),
            pltpu.VMEM((1, width), jnp.float32),
            pltpu.VMEM(ids.shape, jnp.int32),
            pltpu.VMEM(ids.shape, jnp.float32),
            pltpu.VMEM((1, piece), jnp.float32),
            pltpu.VMEM((tok, piece), jnp.bfloat16),
            pltpu.VMEM((slots, tok), jnp.float32),
            dma((5,)),
            pltpu.VMEM((width, hidden), jnp.bfloat16),
            pltpu.VMEM((width, hidden), jnp.bfloat16),
            pltpu.VMEM((hidden, width), jnp.bfloat16),
            pltpu.VMEM((slots, width), jnp.bfloat16),
            pltpu.VMEM((slots, width), jnp.bfloat16),
            pltpu.VMEM((inner - 1, outer, slots, piece), jnp.float32),
            pltpu.VMEM((inner - 1, outer, slots, piece), jnp.float32),
            pltpu.VMEM((outer, slots, piece), jnp.float32),
            pltpu.VMEM((outer, slots, piece), jnp.float32),
            pltpu.VMEM((slots, piece), jnp.float32),
            pltpu.VMEM((slots, piece), jnp.float32),
            pltpu.VMEM((parts, tok, 128), jnp.float32),
            dma((3,)), dma((groups,)), dma((groups,)), dma((groups, parts)), dma((groups, parts)),
            dma((inner - 1, outer)), dma((inner - 1, outer)), dma((outer, groups)), dma((outer, groups)),
            dma((groups,)), dma((groups,)), dma((parts,)), dma((parts,)),
        ],
        compiler_params=pltpu.CompilerParams(collective_id=0, has_side_effects=True),
    )(tokens, in_gain.reshape(1, -1), ids, weights, w_gate, w_up, w_down, out_gain.reshape(1, -1))


def collectives(tokens, in_gain, expert_ids, route_weight, w_gate, w_up, w_down, out_gain):
    tok_rows = tokens.shape[0]
    top_count = expert_ids.shape[1]
    local_experts = w_gate.shape[0]
    groups = lax.axis_size("ep")
    experts = local_experts * groups
    capacity = capacity_of(tok_rows, top_count, local_experts, experts)
    values = tokens.astype(jnp.float32)
    row_centre = jnp.mean(values, axis=1, keepdims=True)
    centered_in = values - row_centre
    spread_in = jnp.mean(centered_in * centered_in, axis=1, keepdims=True)
    normed = (centered_in * lax.rsqrt(spread_in + norm_eps) * in_gain).astype(jnp.bfloat16)
    routes_flat = expert_ids.reshape(-1)
    labels = lax.broadcasted_iota(jnp.int32, (1, experts), 1)
    one_hot = (routes_flat[:, None] == labels).astype(jnp.int32)
    before = jnp.cumsum(one_hot, axis=0) - one_hot
    slot_index = jnp.sum(before * one_hot, axis=1)
    positions = routes_flat * capacity + slot_index
    source = jnp.repeat(normed, top_count, axis=0)
    outgoing = (
        jnp.zeros((experts * capacity, normed.shape[1]), jnp.bfloat16).at[positions].set(source)
    )
    arrived = lax.all_to_all(outgoing, "ep", split_axis=0, concat_axis=0, tiled=True)
    arrived = arrived.reshape(groups, local_experts, capacity, normed.shape[1])
    gate_act = jnp.einsum("sjcd,jdf->sjcf", arrived, w_gate, preferred_element_type=jnp.float32)
    up_act = jnp.einsum("sjcd,jdf->sjcf", arrived, w_up, preferred_element_type=jnp.float32)
    hidden = (jax.nn.silu(gate_act) * up_act).astype(jnp.bfloat16)
    partial_value = jnp.einsum("sjcf,jfd->sjcd", hidden, w_down, preferred_element_type=jnp.float32)
    partial_value = partial_value.reshape(experts * capacity, normed.shape[1])
    weights = route_weight.reshape(-1, 1)

    def combine(returned):
        picked = returned[positions] * weights
        return jnp.sum(picked.reshape(tok_rows, top_count, -1), axis=1)

    summed = lax.psum_scatter(partial_value, "tp", scatter_dimension=1, tiled=True)
    returned = lax.all_to_all(summed, "ep", split_axis=0, concat_axis=0, tiled=True)
    mixture = combine(returned)
    full_width = mixture.shape[1] * lax.axis_size("tp")
    row_total = lax.psum(jnp.sum(mixture, axis=1, keepdims=True), "tp")
    row_mean = row_total / full_width
    centered = mixture - row_mean
    deviations = lax.psum(jnp.sum(centered * centered, axis=1, keepdims=True), "tp")
    spread = deviations / full_width
    return (centered * lax.rsqrt(spread + norm_eps) * out_gain).astype(jnp.bfloat16)


def shards(tokens, in_gain, expert_ids, route_weight, w_gate, w_up, w_down, out_gain):
    groups, parts = lax.axis_size("ep"), lax.axis_size("tp")
    tok_rows, width = tokens.shape
    local_experts = w_gate.shape[0]
    cap = capacity_of(tok_rows, expert_ids.shape[1], local_experts, local_experts * groups)
    whole_tiles = cap % 16 == 0 and (groups * cap) % 128 == 0 and width % (parts * 128) == 0
    if local_experts == 1 and parts % 2 == 0 and whole_tiles and groups * cap * width <= 1 << 20:
        return one_kernel(
            groups, parts, cap, tokens, in_gain, expert_ids.T, route_weight.T, w_gate, w_up, w_down, out_gain
        )
    return collectives(
        tokens, in_gain, expert_ids, route_weight, w_gate, w_up, w_down, out_gain
    )


def solution(mesh):
    in_specs = (
        P("ep", None),
        P(),
        P("ep", None),
        P("ep", None),
        P("ep", None, "tp"),
        P("ep", None, "tp"),
        P("ep", "tp", None),
        P("tp"),
    )
    out_specs = P("ep", "tp")
    return jax.shard_map(shards, mesh=mesh, in_specs=in_specs, out_specs=out_specs, check_vma=False)
```

```python
import functools

import jax
import jax.numpy as jnp
from jax import lax
from jax.experimental import pallas as pl
from jax.experimental.pallas import tpu as pltpu
from jax.sharding import PartitionSpec as P

norm_eps = 1e-05
MESH = pl.DeviceIdType.MESH


def capacity_of(tok_rows, top_count, local_experts, experts):
    return max(
        2, min(tok_rows // (2 * local_experts), (5 * tok_rows * top_count + experts - 1) // experts)
    )


def fused(
    groups, parts, inner, cap,
    tokens_h, in_gain_h, ids_h, weights_h, w_gate, w_up, w_down, out_gain_h,
    out_h,
    tokens, in_gain, ids, weights, out_gain, out, picked, row_sem,
    gate_v, up_v, down_v, sent, arrived, part, half_in, half, quarter_in, reduced, returned, stats,
    w_sem, ep_send, ep_recv, tp_send, tp_recv, in_send, in_recv, out_send, out_recv,
    ret_send, ret_recv, st_send, st_recv,
):
    outer = parts // inner
    ep, tp = lax.axis_index("ep"), lax.axis_index("tp")
    o, i = tp // inner, tp % inner
    tok, width = tokens.shape
    slots = groups * cap
    piece = width // parts

    def rows(g):
        return pl.ds(pl.multiple_of(g * cap, cap), cap)

    def cols(b):
        return pl.ds(pl.multiple_of(b * piece, piece), piece)

    barrier = pltpu.get_barrier_semaphore()
    for off in range(1, groups):
        pl.semaphore_signal(barrier, inc=1, device_id=((ep + off) % groups, tp), device_id_type=MESH)
    for j in range(1, parts):
        pl.semaphore_signal(barrier, inc=1, device_id=(ep, (tp + j) % parts), device_id_type=MESH)

    row_loads = [
        pltpu.make_async_copy(src, dst, row_sem.at[n])
        for n, (src, dst) in enumerate((
            (tokens_h, tokens), (in_gain_h, in_gain), (ids_h, ids), (weights_h, weights),
            (out_gain_h, out_gain),
        ))
    ]
    for load in row_loads:
        load.start()
    loads = [
        pltpu.make_async_copy(src.at[0], dst, w_sem.at[n])
        for n, (src, dst) in enumerate(((w_gate, gate_v), (w_up, up_v), (w_down, down_v)))
    ]
    for load in loads:
        load.start()

    for load in row_loads:
        load.wait()
    values = tokens[...].astype(jnp.float32)
    centred = values - jnp.mean(values, axis=1, keepdims=True)
    spread = jnp.mean(centred * centred, axis=1, keepdims=True)
    normed = (centred * lax.rsqrt(spread + norm_eps) * in_gain[...]).astype(jnp.bfloat16)

    lane = lax.broadcasted_iota(jnp.int32, (slots, tok), 0)
    owner = jnp.zeros((slots, tok), jnp.int32)
    for g in range(1, groups):
        owner = owner + jnp.where(lane >= g * cap, 1, 0)
    slot = (lane - owner * cap).astype(jnp.float32)
    named = jnp.zeros((slots, tok), jnp.float32)
    scale = jnp.zeros((slots, tok), jnp.float32)
    for k in range(ids.shape[0]):
        hit = ids[k:k + 1, :] == owner
        named = named + jnp.where(hit, 1.0, 0.0)
        scale = scale + jnp.where(hit, weights[k:k + 1, :], 0.0)
    earlier = (
        lax.broadcasted_iota(jnp.int32, (tok, tok), 0) < lax.broadcasted_iota(jnp.int32, (tok, tok), 1)
    )
    before = jnp.dot(
        named.astype(jnp.bfloat16), jnp.where(earlier, 1.0, 0.0).astype(jnp.bfloat16),
        preferred_element_type=jnp.float32,
    )
    chosen = jnp.where(before == slot, named, 0.0)
    picked[...] = chosen * scale
    sent[...] = jnp.dot(
        chosen.astype(jnp.bfloat16), normed, preferred_element_type=jnp.float32
    ).astype(jnp.bfloat16)

    pl.semaphore_wait(barrier, groups - 1 + parts - 1)

    order = sorted(range(1, groups), key=lambda off: -min(off, groups - off))
    scatter = {}
    for off in order:
        to = (ep + off) % groups
        scatter[off] = pltpu.make_async_remote_copy(
            src_ref=sent.at[rows(to), cols(tp)], dst_ref=arrived.at[rows(ep), cols(tp)],
            send_sem=ep_send.at[off], recv_sem=ep_recv.at[off],
            device_id=(to, tp), device_id_type=MESH,
        )
        scatter[off].start()
    arrived[rows(ep), :] = sent[rows(ep), :]
    spread_out, relays, local = [], {}, []

    def share(off, block, j, to):
        came = (ep + groups - off) % groups
        copy = pltpu.make_async_remote_copy(
            src_ref=arrived.at[rows(came), cols(block)], dst_ref=arrived.at[rows(came), cols(block)],
            send_sem=tp_send.at[off, j], recv_sem=tp_recv.at[off, j],
            device_id=(ep, to), device_id_type=MESH,
        )
        copy.start()
        spread_out.append(copy)
        return copy

    for off in order:
        scatter[off].wait_recv()
        for a in range(1, outer):
            relays[off, a] = share(off, tp, a * inner, (o + a) % outer * inner + i)
        for b in range(1, inner):
            local.append(share(off, tp, b, o * inner + (i + b) % inner))
    for off in order:
        for a in range(1, outer):
            relays[off, a].wait_recv()
            block = (o + outer - a) % outer * inner + i
            for b in range(1, inner):
                local.append(share(off, block, a * inner + b, o * inner + (i + b) % inner))
    for load in loads:
        load.wait()
    for copy in local:
        copy.wait_recv()

    inputs = arrived[...]
    gate_act = jnp.dot(inputs, gate_v[...], preferred_element_type=jnp.float32)
    up_act = jnp.dot(inputs, up_v[...], preferred_element_type=jnp.float32)
    hidden = (gate_act / (1.0 + jnp.exp(-gate_act)) * up_act).astype(jnp.bfloat16)

    def down(b):
        return jnp.dot(hidden, down_v[:, cols(b)], preferred_element_type=jnp.float32)

    far = [(o + j) % outer for j in range(1, outer)]
    places = far + [o]
    inner_copies = []
    for n in range(1, inner):
        other = (i + n) % inner
        for p, place in enumerate(places):
            part[n - 1, p] = down(place * inner + other)
            copy = pltpu.make_async_remote_copy(
                src_ref=part.at[n - 1, p], dst_ref=half_in.at[n - 1, p],
                send_sem=in_send.at[n - 1, p], recv_sem=in_recv.at[n - 1, p],
                device_id=(ep, o * inner + other), device_id_type=MESH,
            )
            copy.start()
            inner_copies.append(copy)
    for p, place in enumerate(places):
        half[p] = down(place * inner + i)

    targets = order + [0]
    outer_copies = {}
    for p in range(outer - 1):
        for n in range(1, inner):
            inner_copies[(n - 1) * outer + p].wait_recv()
        for off in targets:
            at = rows((ep + off) % groups)
            total = half[p, at]
            for n in range(1, inner):
                total = total + half_in[n - 1, p, at]
            half[p, at] = total
            copy = pltpu.make_async_remote_copy(
                src_ref=half.at[p, at], dst_ref=quarter_in.at[p, at],
                send_sem=out_send.at[p, off], recv_sem=out_recv.at[p, off],
                device_id=(ep, far[p] * inner + i), device_id_type=MESH,
            )
            copy.start()
            outer_copies[p, off] = copy
    for n in range(1, inner):
        inner_copies[(n - 1) * outer + outer - 1].wait_recv()
    back = {}
    for off in targets:
        to = (ep + off) % groups
        at = rows(to)
        total = half[outer - 1, at]
        for n in range(1, inner):
            total = total + half_in[n - 1, outer - 1, at]
        for p in range(outer - 1):
            outer_copies[p, off].wait_recv()
            total = total + quarter_in[p, at]
        if off == 0:
            returned[at] = total
        else:
            reduced[at] = total
            back[off] = pltpu.make_async_remote_copy(
                src_ref=reduced.at[at], dst_ref=returned.at[rows(ep)],
                send_sem=ret_send.at[off], recv_sem=ret_recv.at[off],
                device_id=(to, tp), device_id_type=MESH,
            )
            back[off].start()
    for off in order:
        back[off].wait_recv()

    mixture = jnp.dot(
        picked[...].T, returned[...], precision=lax.Precision.HIGHEST, preferred_element_type=jnp.float32
    )
    own_mean = jnp.mean(mixture, axis=1, keepdims=True)
    own_gap = mixture - own_mean
    own_spread = jnp.sum(own_gap * own_gap, axis=1, keepdims=True)
    column = lax.broadcasted_iota(jnp.int32, (tok, 128), 1)
    stats[0] = jnp.where(column == 0, own_mean, own_spread)
    moments = []
    for j in range(1, parts):
        copy = pltpu.make_async_remote_copy(
            src_ref=stats.at[0], dst_ref=stats.at[j],
            send_sem=st_send.at[j], recv_sem=st_recv.at[j],
            device_id=(ep, (tp + j) % parts), device_id_type=MESH,
        )
        copy.start()
        moments.append(copy)
    for copy in moments:
        copy.wait_recv()
    means = [own_mean] + [stats[j][:, 0:1] for j in range(1, parts)]
    spreads = [own_spread] + [stats[j][:, 1:2] for j in range(1, parts)]
    row_mean = sum(means) / parts
    total = sum(spreads)
    for mean in means:
        total = total + piece * (mean - row_mean) * (mean - row_mean)
    out[...] = (
        (mixture - row_mean) * lax.rsqrt(total / width + norm_eps) * out_gain[...]
    ).astype(out.dtype)
    result = pltpu.make_async_copy(out, out_h, row_sem.at[0])
    result.start()

    for off in order:
        scatter[off].wait_send()
        back[off].wait_send()
    for copy in spread_out + inner_copies + list(outer_copies.values()) + moments:
        copy.wait_send()
    result.wait()


def one_kernel(groups, parts, cap, tokens, in_gain, ids, weights, w_gate, w_up, w_down, out_gain):
    inner = 2
    outer = parts // inner
    tok, width = tokens.shape
    slots, piece, hidden = groups * cap, width // parts, w_gate.shape[2]
    hbm, dma = pl.BlockSpec(memory_space=pl.ANY), pltpu.SemaphoreType.DMA
    return pl.pallas_call(
        functools.partial(fused, groups, parts, inner, cap),
        name="experts",
        out_shape=jax.ShapeDtypeStruct((tok, piece), jnp.bfloat16),
        in_specs=[hbm] * 8,
        out_specs=hbm,
        scratch_shapes=[
            pltpu.VMEM((tok, width), jnp.bfloat16),
            pltpu.VMEM((1, width), jnp.float32),
            pltpu.VMEM(ids.shape, jnp.int32),
            pltpu.VMEM(ids.shape, jnp.float32),
            pltpu.VMEM((1, piece), jnp.float32),
            pltpu.VMEM((tok, piece), jnp.bfloat16),
            pltpu.VMEM((slots, tok), jnp.float32),
            dma((5,)),
            pltpu.VMEM((width, hidden), jnp.bfloat16),
            pltpu.VMEM((width, hidden), jnp.bfloat16),
            pltpu.VMEM((hidden, width), jnp.bfloat16),
            pltpu.VMEM((slots, width), jnp.bfloat16),
            pltpu.VMEM((slots, width), jnp.bfloat16),
            pltpu.VMEM((inner - 1, outer, slots, piece), jnp.float32),
            pltpu.VMEM((inner - 1, outer, slots, piece), jnp.float32),
            pltpu.VMEM((outer, slots, piece), jnp.float32),
            pltpu.VMEM((outer, slots, piece), jnp.float32),
            pltpu.VMEM((slots, piece), jnp.float32),
            pltpu.VMEM((slots, piece), jnp.float32),
            pltpu.VMEM((parts, tok, 128), jnp.float32),
            dma((3,)), dma((groups,)), dma((groups,)), dma((groups, parts)), dma((groups, parts)),
            dma((inner - 1, outer)), dma((inner - 1, outer)), dma((outer, groups)), dma((outer, groups)),
            dma((groups,)), dma((groups,)), dma((parts,)), dma((parts,)),
        ],
        compiler_params=pltpu.CompilerParams(collective_id=0, has_side_effects=True),
    )(tokens, in_gain.reshape(1, -1), ids, weights, w_gate, w_up, w_down, out_gain.reshape(1, -1))


def collectives(tokens, in_gain, expert_ids, route_weight, w_gate, w_up, w_down, out_gain):
    tok_rows = tokens.shape[0]
    top_count = expert_ids.shape[1]
    local_experts = w_gate.shape[0]
    groups = lax.axis_size("ep")
    experts = local_experts * groups
    capacity = capacity_of(tok_rows, top_count, local_experts, experts)
    values = tokens.astype(jnp.float32)
    row_centre = jnp.mean(values, axis=1, keepdims=True)
    centered_in = values - row_centre
    spread_in = jnp.mean(centered_in * centered_in, axis=1, keepdims=True)
    normed = (centered_in * lax.rsqrt(spread_in + norm_eps) * in_gain).astype(jnp.bfloat16)
    routes_flat = expert_ids.reshape(-1)
    labels = lax.broadcasted_iota(jnp.int32, (1, experts), 1)
    one_hot = (routes_flat[:, None] == labels).astype(jnp.int32)
    before = jnp.cumsum(one_hot, axis=0) - one_hot
    slot_index = jnp.sum(before * one_hot, axis=1)
    positions = routes_flat * capacity + slot_index
    source = jnp.repeat(normed, top_count, axis=0)
    outgoing = (
        jnp.zeros((experts * capacity, normed.shape[1]), jnp.bfloat16).at[positions].set(source)
    )
    arrived = lax.all_to_all(outgoing, "ep", split_axis=0, concat_axis=0, tiled=True)
    arrived = arrived.reshape(groups, local_experts, capacity, normed.shape[1])
    gate_act = jnp.einsum("sjcd,jdf->sjcf", arrived, w_gate, preferred_element_type=jnp.float32)
    up_act = jnp.einsum("sjcd,jdf->sjcf", arrived, w_up, preferred_element_type=jnp.float32)
    hidden = (jax.nn.silu(gate_act) * up_act).astype(jnp.bfloat16)
    partial_value = jnp.einsum("sjcf,jfd->sjcd", hidden, w_down, preferred_element_type=jnp.float32)
    partial_value = partial_value.reshape(experts * capacity, normed.shape[1])
    weights = route_weight.reshape(-1, 1)

    def combine(returned):
        picked = returned[positions] * weights
        return jnp.sum(picked.reshape(tok_rows, top_count, -1), axis=1)

    summed = lax.psum_scatter(partial_value, "tp", scatter_dimension=1, tiled=True)
    returned = lax.all_to_all(summed, "ep", split_axis=0, concat_axis=0, tiled=True)
    mixture = combine(returned)
    full_width = mixture.shape[1] * lax.axis_size("tp")
    row_total = lax.psum(jnp.sum(mixture, axis=1, keepdims=True), "tp")
    row_mean = row_total / full_width
    centered = mixture - row_mean
    deviations = lax.psum(jnp.sum(centered * centered, axis=1, keepdims=True), "tp")
    spread = deviations / full_width
    return (centered * lax.rsqrt(spread + norm_eps) * out_gain).astype(jnp.bfloat16)


def shards(tokens, in_gain, expert_ids, route_weight, w_gate, w_up, w_down, out_gain):
    groups, parts = lax.axis_size("ep"), lax.axis_size("tp")
    tok_rows, width = tokens.shape
    local_experts = w_gate.shape[0]
    cap = capacity_of(tok_rows, expert_ids.shape[1], local_experts, local_experts * groups)
    whole_tiles = cap % 16 == 0 and (groups * cap) % 128 == 0 and width % (parts * 128) == 0
    if local_experts == 1 and parts % 2 == 0 and whole_tiles and groups * cap * width <= 1 << 20:
        return one_kernel(
            groups, parts, cap, tokens, in_gain, expert_ids.T, route_weight.T, w_gate, w_up, w_down, out_gain
        )
    return collectives(
        tokens, in_gain, expert_ids, route_weight, w_gate, w_up, w_down, out_gain
    )


def solution(mesh):
    in_specs = (
        P("ep", None),
        P(),
        P("ep", None),
        P("ep", None),
        P("ep", None, "tp"),
        P("ep", None, "tp"),
        P("ep", "tp", None),
        P("tp"),
    )
    out_specs = P("ep", "tp")
    return jax.shard_map(shards, mesh=mesh, in_specs=in_specs, out_specs=out_specs, check_vma=False)
```

```python
import functools

import jax
import jax.numpy as jnp
from jax import lax
from jax.experimental import pallas as pl
from jax.experimental.pallas import tpu as pltpu
from jax.sharding import PartitionSpec as P

norm_eps = 1e-05
MESH = pl.DeviceIdType.MESH


def capacity_of(tok_rows, top_count, local_experts, experts):
    return max(
        2, min(tok_rows // (2 * local_experts), (5 * tok_rows * top_count + experts - 1) // experts)
    )


def encode(values):
    peak = jnp.maximum(jnp.max(jnp.abs(values), axis=1, keepdims=True), 2.0 ** -100)
    power = jnp.floor(jnp.log2(peak)) - 14.0
    whole = jnp.clip(jnp.round(values * jnp.exp2(-power)), -32767.0, 32767.0)
    power = jnp.broadcast_to(power, (values.shape[0], 128))
    return jnp.concatenate([whole, power], axis=1).astype(jnp.int32).astype(jnp.int16)


def decode(code):
    code = code.astype(jnp.int32).astype(jnp.float32)
    return code[:, :-128] * jnp.exp2(code[:, -128:-127])


def fused(
    groups, parts, inner, cap,
    tokens_h, in_gain_h, ids_h, weights_h, w_gate, w_up, w_down, out_gain_h,
    out_h,
    tokens, in_gain, ids, weights, out_gain, out, picked, row_sem,
    gate_v, up_v, down_v, sent, arrived, part, half_in, half, quarter, quarter_in, reduced, returned, stats,
    w_sem, ep_send, ep_recv, tp_send, tp_recv, in_send, in_recv, out_send, out_recv,
    ret_send, ret_recv, st_send, st_recv,
):
    outer = parts // inner
    ep, tp = lax.axis_index("ep"), lax.axis_index("tp")
    o, i = tp // inner, tp % inner
    tok, width = tokens.shape
    slots = groups * cap
    piece = width // parts

    def rows(g):
        return pl.ds(pl.multiple_of(g * cap, cap), cap)

    def cols(b):
        return pl.ds(pl.multiple_of(b * piece, piece), piece)

    barrier = pltpu.get_barrier_semaphore()
    for off in range(1, groups):
        pl.semaphore_signal(barrier, inc=1, device_id=((ep + off) % groups, tp), device_id_type=MESH)
    for j in range(1, parts):
        pl.semaphore_signal(barrier, inc=1, device_id=(ep, (tp + j) % parts), device_id_type=MESH)

    row_loads = [
        pltpu.make_async_copy(src, dst, row_sem.at[n])
        for n, (src, dst) in enumerate((
            (tokens_h, tokens), (in_gain_h, in_gain), (ids_h, ids), (weights_h, weights),
            (out_gain_h, out_gain),
        ))
    ]
    for load in row_loads:
        load.start()
    loads = [
        pltpu.make_async_copy(src.at[0], dst, w_sem.at[n])
        for n, (src, dst) in enumerate(((w_gate, gate_v), (w_up, up_v), (w_down, down_v)))
    ]
    for load in loads:
        load.start()

    for load in row_loads:
        load.wait()
    values = tokens[...].astype(jnp.float32)
    centred = values - jnp.mean(values, axis=1, keepdims=True)
    spread = jnp.mean(centred * centred, axis=1, keepdims=True)
    normed = (centred * lax.rsqrt(spread + norm_eps) * in_gain[...]).astype(jnp.bfloat16)

    lane = lax.broadcasted_iota(jnp.int32, (slots, tok), 0)
    owner = jnp.zeros((slots, tok), jnp.int32)
    for g in range(1, groups):
        owner = owner + jnp.where(lane >= g * cap, 1, 0)
    slot = (lane - owner * cap).astype(jnp.float32)
    named = jnp.zeros((slots, tok), jnp.float32)
    scale = jnp.zeros((slots, tok), jnp.float32)
    for k in range(ids.shape[0]):
        hit = ids[k:k + 1, :] == owner
        named = named + jnp.where(hit, 1.0, 0.0)
        scale = scale + jnp.where(hit, weights[k:k + 1, :], 0.0)
    earlier = (
        lax.broadcasted_iota(jnp.int32, (tok, tok), 0) < lax.broadcasted_iota(jnp.int32, (tok, tok), 1)
    )
    before = jnp.dot(
        named.astype(jnp.bfloat16), jnp.where(earlier, 1.0, 0.0).astype(jnp.bfloat16),
        preferred_element_type=jnp.float32,
    )
    chosen = jnp.where(before == slot, named, 0.0)
    picked[...] = chosen * scale
    sent[...] = jnp.dot(
        chosen.astype(jnp.bfloat16), normed, preferred_element_type=jnp.float32
    ).astype(jnp.bfloat16)

    pl.semaphore_wait(barrier, groups - 1 + parts - 1)

    order = sorted(range(1, groups), key=lambda off: -min(off, groups - off))
    scatter = {}
    for off in order:
        to = (ep + off) % groups
        scatter[off] = pltpu.make_async_remote_copy(
            src_ref=sent.at[rows(to), cols(tp)], dst_ref=arrived.at[rows(ep), cols(tp)],
            send_sem=ep_send.at[off], recv_sem=ep_recv.at[off],
            device_id=(to, tp), device_id_type=MESH,
        )
        scatter[off].start()
    arrived[rows(ep), :] = sent[rows(ep), :]
    spread_out, relays, local = [], {}, []

    def share(off, block, j, to):
        came = (ep + groups - off) % groups
        copy = pltpu.make_async_remote_copy(
            src_ref=arrived.at[rows(came), cols(block)], dst_ref=arrived.at[rows(came), cols(block)],
            send_sem=tp_send.at[off, j], recv_sem=tp_recv.at[off, j],
            device_id=(ep, to), device_id_type=MESH,
        )
        copy.start()
        spread_out.append(copy)
        return copy

    for off in order:
        scatter[off].wait_recv()
        for a in range(1, outer):
            relays[off, a] = share(off, tp, a * inner, (o + a) % outer * inner + i)
        for b in range(1, inner):
            local.append(share(off, tp, b, o * inner + (i + b) % inner))
    for off in order:
        for a in range(1, outer):
            relays[off, a].wait_recv()
            block = (o + outer - a) % outer * inner + i
            for b in range(1, inner):
                local.append(share(off, block, a * inner + b, o * inner + (i + b) % inner))
    for load in loads:
        load.wait()
    for copy in local:
        copy.wait_recv()

    inputs = arrived[...]
    gate_act = jnp.dot(inputs, gate_v[...], preferred_element_type=jnp.float32)
    up_act = jnp.dot(inputs, up_v[...], preferred_element_type=jnp.float32)
    hidden = (gate_act / (1.0 + jnp.exp(-gate_act)) * up_act).astype(jnp.bfloat16)

    def down(b):
        return jnp.dot(hidden, down_v[:, cols(b)], preferred_element_type=jnp.float32)

    far = [(o + j) % outer for j in range(1, outer)]
    places = far + [o]
    inner_copies = []
    for n in range(1, inner):
        other = (i + n) % inner
        for p, place in enumerate(places):
            part[n - 1, p] = down(place * inner + other)
            copy = pltpu.make_async_remote_copy(
                src_ref=part.at[n - 1, p], dst_ref=half_in.at[n - 1, p],
                send_sem=in_send.at[n - 1, p], recv_sem=in_recv.at[n - 1, p],
                device_id=(ep, o * inner + other), device_id_type=MESH,
            )
            copy.start()
            inner_copies.append(copy)
    for p, place in enumerate(places):
        half[p] = down(place * inner + i)

    targets = order + [0]
    outer_copies = {}
    for p in range(outer - 1):
        for n in range(1, inner):
            inner_copies[(n - 1) * outer + p].wait_recv()
        for off in targets:
            at = rows((ep + off) % groups)
            total = half[p, at]
            for n in range(1, inner):
                total = total + half_in[n - 1, p, at]
            quarter[p, at] = encode(total)
            copy = pltpu.make_async_remote_copy(
                src_ref=quarter.at[p, at], dst_ref=quarter_in.at[p, at],
                send_sem=out_send.at[p, off], recv_sem=out_recv.at[p, off],
                device_id=(ep, far[p] * inner + i), device_id_type=MESH,
            )
            copy.start()
            outer_copies[p, off] = copy
    for n in range(1, inner):
        inner_copies[(n - 1) * outer + outer - 1].wait_recv()
    back = {}
    for off in targets:
        to = (ep + off) % groups
        at = rows(to)
        total = half[outer - 1, at]
        for n in range(1, inner):
            total = total + half_in[n - 1, outer - 1, at]
        for p in range(outer - 1):
            outer_copies[p, off].wait_recv()
            total = total + decode(quarter_in[p, at])
        if off == 0:
            returned[at] = encode(total)
        else:
            reduced[at] = encode(total)
            back[off] = pltpu.make_async_remote_copy(
                src_ref=reduced.at[at], dst_ref=returned.at[rows(ep)],
                send_sem=ret_send.at[off], recv_sem=ret_recv.at[off],
                device_id=(to, tp), device_id_type=MESH,
            )
            back[off].start()
    for off in order:
        back[off].wait_recv()

    mixture = jnp.dot(
        picked[...].T, decode(returned[...]), precision=lax.Precision.HIGHEST, preferred_element_type=jnp.float32
    )
    own_mean = jnp.mean(mixture, axis=1, keepdims=True)
    own_gap = mixture - own_mean
    own_spread = jnp.sum(own_gap * own_gap, axis=1, keepdims=True)
    column = lax.broadcasted_iota(jnp.int32, (tok, 128), 1)
    stats[0] = jnp.where(column == 0, own_mean, own_spread)
    moments = []
    for j in range(1, parts):
        copy = pltpu.make_async_remote_copy(
            src_ref=stats.at[0], dst_ref=stats.at[j],
            send_sem=st_send.at[j], recv_sem=st_recv.at[j],
            device_id=(ep, (tp + j) % parts), device_id_type=MESH,
        )
        copy.start()
        moments.append(copy)
    for copy in moments:
        copy.wait_recv()
    means = [own_mean] + [stats[j][:, 0:1] for j in range(1, parts)]
    spreads = [own_spread] + [stats[j][:, 1:2] for j in range(1, parts)]
    row_mean = sum(means) / parts
    total = sum(spreads)
    for mean in means:
        total = total + piece * (mean - row_mean) * (mean - row_mean)
    out[...] = (
        (mixture - row_mean) * lax.rsqrt(total / width + norm_eps) * out_gain[...]
    ).astype(out.dtype)
    result = pltpu.make_async_copy(out, out_h, row_sem.at[0])
    result.start()

    for off in order:
        scatter[off].wait_send()
        back[off].wait_send()
    for copy in spread_out + inner_copies + list(outer_copies.values()) + moments:
        copy.wait_send()
    result.wait()


def one_kernel(groups, parts, cap, tokens, in_gain, ids, weights, w_gate, w_up, w_down, out_gain):
    inner = 2
    outer = parts // inner
    tok, width = tokens.shape
    slots, piece, hidden = groups * cap, width // parts, w_gate.shape[2]
    hbm, dma = pl.BlockSpec(memory_space=pl.ANY), pltpu.SemaphoreType.DMA
    return pl.pallas_call(
        functools.partial(fused, groups, parts, inner, cap),
        name="experts",
        out_shape=jax.ShapeDtypeStruct((tok, piece), jnp.bfloat16),
        in_specs=[hbm] * 8,
        out_specs=hbm,
        scratch_shapes=[
            pltpu.VMEM((tok, width), jnp.bfloat16),
            pltpu.VMEM((1, width), jnp.float32),
            pltpu.VMEM(ids.shape, jnp.int32),
            pltpu.VMEM(ids.shape, jnp.float32),
            pltpu.VMEM((1, piece), jnp.float32),
            pltpu.VMEM((tok, piece), jnp.bfloat16),
            pltpu.VMEM((slots, tok), jnp.float32),
            dma((5,)),
            pltpu.VMEM((width, hidden), jnp.bfloat16),
            pltpu.VMEM((width, hidden), jnp.bfloat16),
            pltpu.VMEM((hidden, width), jnp.bfloat16),
            pltpu.VMEM((slots, width), jnp.bfloat16),
            pltpu.VMEM((slots, width), jnp.bfloat16),
            pltpu.VMEM((inner - 1, outer, slots, piece), jnp.float32),
            pltpu.VMEM((inner - 1, outer, slots, piece), jnp.float32),
            pltpu.VMEM((outer, slots, piece), jnp.float32),
            pltpu.VMEM((outer, slots, piece + 128), jnp.int16),
            pltpu.VMEM((outer, slots, piece + 128), jnp.int16),
            pltpu.VMEM((slots, piece + 128), jnp.int16),
            pltpu.VMEM((slots, piece + 128), jnp.int16),
            pltpu.VMEM((parts, tok, 128), jnp.float32),
            dma((3,)), dma((groups,)), dma((groups,)), dma((groups, parts)), dma((groups, parts)),
            dma((inner - 1, outer)), dma((inner - 1, outer)), dma((outer, groups)), dma((outer, groups)),
            dma((groups,)), dma((groups,)), dma((parts,)), dma((parts,)),
        ],
        compiler_params=pltpu.CompilerParams(collective_id=0, has_side_effects=True),
    )(tokens, in_gain.reshape(1, -1), ids, weights, w_gate, w_up, w_down, out_gain.reshape(1, -1))


def collectives(tokens, in_gain, expert_ids, route_weight, w_gate, w_up, w_down, out_gain):
    tok_rows = tokens.shape[0]
    top_count = expert_ids.shape[1]
    local_experts = w_gate.shape[0]
    groups = lax.axis_size("ep")
    experts = local_experts * groups
    capacity = capacity_of(tok_rows, top_count, local_experts, experts)
    values = tokens.astype(jnp.float32)
    row_centre = jnp.mean(values, axis=1, keepdims=True)
    centered_in = values - row_centre
    spread_in = jnp.mean(centered_in * centered_in, axis=1, keepdims=True)
    normed = (centered_in * lax.rsqrt(spread_in + norm_eps) * in_gain).astype(jnp.bfloat16)
    routes_flat = expert_ids.reshape(-1)
    labels = lax.broadcasted_iota(jnp.int32, (1, experts), 1)
    one_hot = (routes_flat[:, None] == labels).astype(jnp.int32)
    before = jnp.cumsum(one_hot, axis=0) - one_hot
    slot_index = jnp.sum(before * one_hot, axis=1)
    positions = routes_flat * capacity + slot_index
    source = jnp.repeat(normed, top_count, axis=0)
    outgoing = (
        jnp.zeros((experts * capacity, normed.shape[1]), jnp.bfloat16).at[positions].set(source)
    )
    arrived = lax.all_to_all(outgoing, "ep", split_axis=0, concat_axis=0, tiled=True)
    arrived = arrived.reshape(groups, local_experts, capacity, normed.shape[1])
    gate_act = jnp.einsum("sjcd,jdf->sjcf", arrived, w_gate, preferred_element_type=jnp.float32)
    up_act = jnp.einsum("sjcd,jdf->sjcf", arrived, w_up, preferred_element_type=jnp.float32)
    hidden = (jax.nn.silu(gate_act) * up_act).astype(jnp.bfloat16)
    partial_value = jnp.einsum("sjcf,jfd->sjcd", hidden, w_down, preferred_element_type=jnp.float32)
    partial_value = partial_value.reshape(experts * capacity, normed.shape[1])
    weights = route_weight.reshape(-1, 1)

    def combine(returned):
        picked = returned[positions] * weights
        return jnp.sum(picked.reshape(tok_rows, top_count, -1), axis=1)

    summed = lax.psum_scatter(partial_value, "tp", scatter_dimension=1, tiled=True)
    returned = lax.all_to_all(summed, "ep", split_axis=0, concat_axis=0, tiled=True)
    mixture = combine(returned)
    full_width = mixture.shape[1] * lax.axis_size("tp")
    row_total = lax.psum(jnp.sum(mixture, axis=1, keepdims=True), "tp")
    row_mean = row_total / full_width
    centered = mixture - row_mean
    deviations = lax.psum(jnp.sum(centered * centered, axis=1, keepdims=True), "tp")
    spread = deviations / full_width
    return (centered * lax.rsqrt(spread + norm_eps) * out_gain).astype(jnp.bfloat16)


def shards(tokens, in_gain, expert_ids, route_weight, w_gate, w_up, w_down, out_gain):
    groups, parts = lax.axis_size("ep"), lax.axis_size("tp")
    tok_rows, width = tokens.shape
    local_experts = w_gate.shape[0]
    cap = capacity_of(tok_rows, expert_ids.shape[1], local_experts, local_experts * groups)
    whole_tiles = cap % 16 == 0 and (groups * cap) % 128 == 0 and width % (parts * 128) == 0
    if local_experts == 1 and parts % 2 == 0 and whole_tiles and groups * cap * width <= 1 << 20:
        return one_kernel(
            groups, parts, cap, tokens, in_gain, expert_ids.T, route_weight.T, w_gate, w_up, w_down, out_gain
        )
    return collectives(
        tokens, in_gain, expert_ids, route_weight, w_gate, w_up, w_down, out_gain
    )


def solution(mesh):
    in_specs = (
        P("ep", None),
        P(),
        P("ep", None),
        P("ep", None),
        P("ep", None, "tp"),
        P("ep", None, "tp"),
        P("ep", "tp", None),
        P("tp"),
    )
    out_specs = P("ep", "tp")
    return jax.shard_map(shards, mesh=mesh, in_specs=in_specs, out_specs=out_specs, check_vma=False)
```

```python
import functools

import jax
import jax.numpy as jnp
from jax import lax
from jax.experimental import pallas as pl
from jax.experimental.pallas import tpu as pltpu
from jax.sharding import PartitionSpec as P

norm_eps = 1e-05
MESH = pl.DeviceIdType.MESH


def capacity_of(tok_rows, top_count, local_experts, experts):
    return max(
        2, min(tok_rows // (2 * local_experts), (5 * tok_rows * top_count + experts - 1) // experts)
    )


def encode(values):
    peak = jnp.maximum(jnp.max(jnp.abs(values), axis=1, keepdims=True), 2.0 ** -100)
    power = jnp.floor(jnp.log2(peak)) - 14.0
    whole = jnp.clip(jnp.round(values * jnp.exp2(-power)), -32767.0, 32767.0)
    power = jnp.broadcast_to(power, (values.shape[0], 128))
    return jnp.concatenate([whole, power], axis=1).astype(jnp.int32).astype(jnp.int16)


def decode(code):
    code = code.astype(jnp.int32).astype(jnp.float32)
    return code[:, :-128] * jnp.exp2(code[:, -128:-127])


def fused(
    groups, parts, inner, cap,
    tokens_h, in_gain_h, ids_h, weights_h, w_gate, w_up, w_down, out_gain_h,
    out_h,
    tokens, in_gain, ids, weights, out_gain, out, picked, row_sem,
    gate_v, up_v, down_v, sent, arrived, part, half_in, half, quarter, quarter_in, reduced, returned, stats,
    w_sem, ep_send, ep_recv, tp_send, tp_recv, in_send, in_recv, out_send, out_recv,
    ret_send, ret_recv, st_send, st_recv,
):
    outer = parts // inner
    ep, tp = lax.axis_index("ep"), lax.axis_index("tp")
    o, i = tp // inner, tp % inner
    tok, width = tokens.shape
    slots = groups * cap
    piece = width // parts

    def rows(g):
        return pl.ds(pl.multiple_of(g * cap, cap), cap)

    def cols(b):
        return pl.ds(pl.multiple_of(b * piece, piece), piece)

    barrier = pltpu.get_barrier_semaphore()
    for off in range(1, groups):
        pl.semaphore_signal(barrier, inc=1, device_id=((ep + off) % groups, tp), device_id_type=MESH)
    for j in range(1, parts):
        pl.semaphore_signal(barrier, inc=1, device_id=(ep, (tp + j) % parts), device_id_type=MESH)

    row_loads = [
        pltpu.make_async_copy(src, dst, row_sem.at[n])
        for n, (src, dst) in enumerate((
            (tokens_h, tokens), (in_gain_h, in_gain), (ids_h, ids), (weights_h, weights),
            (out_gain_h, out_gain),
        ))
    ]
    for load in row_loads:
        load.start()
    loads = [
        pltpu.make_async_copy(src.at[0], dst, w_sem.at[n])
        for n, (src, dst) in enumerate(((w_gate, gate_v), (w_up, up_v), (w_down, down_v)))
    ]
    for load in loads:
        load.start()

    for load in row_loads:
        load.wait()
    values = tokens[...].astype(jnp.float32)
    centred = values - jnp.mean(values, axis=1, keepdims=True)
    spread = jnp.mean(centred * centred, axis=1, keepdims=True)
    normed = (centred * lax.rsqrt(spread + norm_eps) * in_gain[...]).astype(jnp.bfloat16)

    lane = lax.broadcasted_iota(jnp.int32, (slots, tok), 0)
    owner = jnp.zeros((slots, tok), jnp.int32)
    for g in range(1, groups):
        owner = owner + jnp.where(lane >= g * cap, 1, 0)
    slot = (lane - owner * cap).astype(jnp.float32)
    named = jnp.zeros((slots, tok), jnp.float32)
    scale = jnp.zeros((slots, tok), jnp.float32)
    for k in range(ids.shape[0]):
        hit = ids[k:k + 1, :] == owner
        named = named + jnp.where(hit, 1.0, 0.0)
        scale = scale + jnp.where(hit, weights[k:k + 1, :], 0.0)
    earlier = (
        lax.broadcasted_iota(jnp.int32, (tok, tok), 0) < lax.broadcasted_iota(jnp.int32, (tok, tok), 1)
    )
    before = jnp.dot(
        named.astype(jnp.bfloat16), jnp.where(earlier, 1.0, 0.0).astype(jnp.bfloat16),
        preferred_element_type=jnp.float32,
    )
    chosen = jnp.where(before == slot, named, 0.0)
    picked[...] = chosen * scale
    sent[...] = jnp.dot(
        chosen.astype(jnp.bfloat16), normed, preferred_element_type=jnp.float32
    ).astype(jnp.bfloat16)

    pl.semaphore_wait(barrier, groups - 1 + parts - 1)

    order = sorted(range(1, groups), key=lambda off: -min(off, groups - off))
    scatter = {}
    for off in order:
        to = (ep + off) % groups
        scatter[off] = pltpu.make_async_remote_copy(
            src_ref=sent.at[rows(to), cols(tp)], dst_ref=arrived.at[rows(ep), cols(tp)],
            send_sem=ep_send.at[off], recv_sem=ep_recv.at[off],
            device_id=(to, tp), device_id_type=MESH,
        )
        scatter[off].start()
    arrived[rows(ep), :] = sent[rows(ep), :]
    spread_out, relays, local = [], {}, []

    def share(off, block, j, to):
        came = (ep + groups - off) % groups
        copy = pltpu.make_async_remote_copy(
            src_ref=arrived.at[rows(came), cols(block)], dst_ref=arrived.at[rows(came), cols(block)],
            send_sem=tp_send.at[off, j], recv_sem=tp_recv.at[off, j],
            device_id=(ep, to), device_id_type=MESH,
        )
        copy.start()
        spread_out.append(copy)
        return copy

    for off in order:
        scatter[off].wait_recv()
        for a in range(1, outer):
            relays[off, a] = share(off, tp, a * inner, (o + a) % outer * inner + i)
        for b in range(1, inner):
            local.append(share(off, tp, b, o * inner + (i + b) % inner))
    for off in order:
        for a in range(1, outer):
            relays[off, a].wait_recv()
            block = (o + outer - a) % outer * inner + i
            for b in range(1, inner):
                local.append(share(off, block, a * inner + b, o * inner + (i + b) % inner))
    for load in loads:
        load.wait()
    for copy in local:
        copy.wait_recv()

    inputs = arrived[...]
    gate_act = jnp.dot(inputs, gate_v[...], preferred_element_type=jnp.float32)
    up_act = jnp.dot(inputs, up_v[...], preferred_element_type=jnp.float32)
    hidden = (gate_act / (1.0 + jnp.exp(-gate_act)) * up_act).astype(jnp.bfloat16)

    def down(b):
        return jnp.dot(hidden, down_v[:, cols(b)], preferred_element_type=jnp.float32)

    far = [(o + j) % outer for j in range(1, outer)]
    places = far + [o]
    halves = {}
    for p, place in enumerate(places):
        for n in range(1, inner):
            other = (i + n) % inner
            part[n - 1, p] = down(place * inner + other)
            halves[n, p] = pltpu.make_async_remote_copy(
                src_ref=part.at[n - 1, p], dst_ref=half_in.at[n - 1, p],
                send_sem=in_send.at[n - 1, p], recv_sem=in_recv.at[n - 1, p],
                device_id=(ep, o * inner + other), device_id_type=MESH,
            )
            halves[n, p].start()
        if p < outer - 1:
            half[p] = down(place * inner + i)
    inner_copies = list(halves.values())

    targets = order + [0]
    outer_copies = {}
    for p in range(outer - 1):
        for n in range(1, inner):
            halves[n, p].wait_recv()
        total = half[p]
        for n in range(1, inner):
            total = total + half_in[n - 1, p]
        quarter[p] = encode(total)
        for off in targets:
            at = rows((ep + off) % groups)
            copy = pltpu.make_async_remote_copy(
                src_ref=quarter.at[p, at], dst_ref=quarter_in.at[p, at],
                send_sem=out_send.at[p, off], recv_sem=out_recv.at[p, off],
                device_id=(ep, far[p] * inner + i), device_id_type=MESH,
            )
            copy.start()
            outer_copies[p, off] = copy
    half[outer - 1] = down(o * inner + i)
    for n in range(1, inner):
        halves[n, outer - 1].wait_recv()
    back = {}
    for off in targets:
        to = (ep + off) % groups
        at = rows(to)
        total = half[outer - 1, at]
        for n in range(1, inner):
            total = total + half_in[n - 1, outer - 1, at]
        for p in range(outer - 1):
            outer_copies[p, off].wait_recv()
            total = total + decode(quarter_in[p, at])
        if off == 0:
            returned[at] = encode(total)
        else:
            reduced[at] = encode(total)
            back[off] = pltpu.make_async_remote_copy(
                src_ref=reduced.at[at], dst_ref=returned.at[rows(ep)],
                send_sem=ret_send.at[off], recv_sem=ret_recv.at[off],
                device_id=(to, tp), device_id_type=MESH,
            )
            back[off].start()
    for off in order:
        back[off].wait_recv()

    mixture = jnp.dot(
        picked[...].T, decode(returned[...]), precision=lax.Precision.HIGHEST, preferred_element_type=jnp.float32
    )
    own_mean = jnp.mean(mixture, axis=1, keepdims=True)
    own_gap = mixture - own_mean
    own_spread = jnp.sum(own_gap * own_gap, axis=1, keepdims=True)
    column = lax.broadcasted_iota(jnp.int32, (tok, 128), 1)
    stats[0] = jnp.where(column == 0, own_mean, own_spread).T[0:8, :]
    moments = []
    for j in range(1, parts):
        copy = pltpu.make_async_remote_copy(
            src_ref=stats.at[0], dst_ref=stats.at[j],
            send_sem=st_send.at[j], recv_sem=st_recv.at[j],
            device_id=(ep, (tp + j) % parts), device_id_type=MESH,
        )
        copy.start()
        moments.append(copy)
    for copy in moments:
        copy.wait_recv()
    means = [stats[j][0:1, :] for j in range(parts)]
    spreads = [stats[j][1:2, :] for j in range(parts)]
    row_mean = sum(means) / parts
    total = sum(spreads)
    for mean in means:
        total = total + piece * (mean - row_mean) * (mean - row_mean)
    factor = lax.rsqrt(total / width + norm_eps)
    line = lax.broadcasted_iota(jnp.int32, (8, tok), 0)
    both = jnp.where(line == 0, row_mean, factor).T
    out[...] = (
        (mixture - both[:, 0:1]) * both[:, 1:2] * out_gain[...]
    ).astype(out.dtype)
    result = pltpu.make_async_copy(out, out_h, row_sem.at[0])
    result.start()

    for off in order:
        scatter[off].wait_send()
        back[off].wait_send()
    for copy in spread_out + inner_copies + list(outer_copies.values()) + moments:
        copy.wait_send()
    result.wait()


def one_kernel(groups, parts, cap, tokens, in_gain, ids, weights, w_gate, w_up, w_down, out_gain):
    inner = 2
    outer = parts // inner
    tok, width = tokens.shape
    slots, piece, hidden = groups * cap, width // parts, w_gate.shape[2]
    hbm, dma = pl.BlockSpec(memory_space=pl.ANY), pltpu.SemaphoreType.DMA
    return pl.pallas_call(
        functools.partial(fused, groups, parts, inner, cap),
        name="experts",
        out_shape=jax.ShapeDtypeStruct((tok, piece), jnp.bfloat16),
        in_specs=[hbm] * 8,
        out_specs=hbm,
        scratch_shapes=[
            pltpu.VMEM((tok, width), jnp.bfloat16),
            pltpu.VMEM((1, width), jnp.float32),
            pltpu.VMEM(ids.shape, jnp.int32),
            pltpu.VMEM(ids.shape, jnp.float32),
            pltpu.VMEM((1, piece), jnp.float32),
            pltpu.VMEM((tok, piece), jnp.bfloat16),
            pltpu.VMEM((slots, tok), jnp.float32),
            dma((5,)),
            pltpu.VMEM((width, hidden), jnp.bfloat16),
            pltpu.VMEM((width, hidden), jnp.bfloat16),
            pltpu.VMEM((hidden, width), jnp.bfloat16),
            pltpu.VMEM((slots, width), jnp.bfloat16),
            pltpu.VMEM((slots, width), jnp.bfloat16),
            pltpu.VMEM((inner - 1, outer, slots, piece), jnp.float32),
            pltpu.VMEM((inner - 1, outer, slots, piece), jnp.float32),
            pltpu.VMEM((outer, slots, piece), jnp.float32),
            pltpu.VMEM((outer, slots, piece + 128), jnp.int16),
            pltpu.VMEM((outer, slots, piece + 128), jnp.int16),
            pltpu.VMEM((slots, piece + 128), jnp.int16),
            pltpu.VMEM((slots, piece + 128), jnp.int16),
            pltpu.VMEM((parts, 8, tok), jnp.float32),
            dma((3,)), dma((groups,)), dma((groups,)), dma((groups, parts)), dma((groups, parts)),
            dma((inner - 1, outer)), dma((inner - 1, outer)), dma((outer, groups)), dma((outer, groups)),
            dma((groups,)), dma((groups,)), dma((parts,)), dma((parts,)),
        ],
        compiler_params=pltpu.CompilerParams(collective_id=0, has_side_effects=True),
    )(tokens, in_gain.reshape(1, -1), ids, weights, w_gate, w_up, w_down, out_gain.reshape(1, -1))


def collectives(tokens, in_gain, expert_ids, route_weight, w_gate, w_up, w_down, out_gain):
    tok_rows = tokens.shape[0]
    top_count = expert_ids.shape[1]
    local_experts = w_gate.shape[0]
    groups = lax.axis_size("ep")
    experts = local_experts * groups
    capacity = capacity_of(tok_rows, top_count, local_experts, experts)
    values = tokens.astype(jnp.float32)
    row_centre = jnp.mean(values, axis=1, keepdims=True)
    centered_in = values - row_centre
    spread_in = jnp.mean(centered_in * centered_in, axis=1, keepdims=True)
    normed = (centered_in * lax.rsqrt(spread_in + norm_eps) * in_gain).astype(jnp.bfloat16)
    routes_flat = expert_ids.reshape(-1)
    labels = lax.broadcasted_iota(jnp.int32, (1, experts), 1)
    one_hot = (routes_flat[:, None] == labels).astype(jnp.int32)
    before = jnp.cumsum(one_hot, axis=0) - one_hot
    slot_index = jnp.sum(before * one_hot, axis=1)
    positions = routes_flat * capacity + slot_index
    source = jnp.repeat(normed, top_count, axis=0)
    outgoing = (
        jnp.zeros((experts * capacity, normed.shape[1]), jnp.bfloat16).at[positions].set(source)
    )
    arrived = lax.all_to_all(outgoing, "ep", split_axis=0, concat_axis=0, tiled=True)
    arrived = arrived.reshape(groups, local_experts, capacity, normed.shape[1])
    gate_act = jnp.einsum("sjcd,jdf->sjcf", arrived, w_gate, preferred_element_type=jnp.float32)
    up_act = jnp.einsum("sjcd,jdf->sjcf", arrived, w_up, preferred_element_type=jnp.float32)
    hidden = (jax.nn.silu(gate_act) * up_act).astype(jnp.bfloat16)
    partial_value = jnp.einsum("sjcf,jfd->sjcd", hidden, w_down, preferred_element_type=jnp.float32)
    partial_value = partial_value.reshape(experts * capacity, normed.shape[1])
    weights = route_weight.reshape(-1, 1)

    def combine(returned):
        picked = returned[positions] * weights
        return jnp.sum(picked.reshape(tok_rows, top_count, -1), axis=1)

    summed = lax.psum_scatter(partial_value, "tp", scatter_dimension=1, tiled=True)
    returned = lax.all_to_all(summed, "ep", split_axis=0, concat_axis=0, tiled=True)
    mixture = combine(returned)
    full_width = mixture.shape[1] * lax.axis_size("tp")
    row_total = lax.psum(jnp.sum(mixture, axis=1, keepdims=True), "tp")
    row_mean = row_total / full_width
    centered = mixture - row_mean
    deviations = lax.psum(jnp.sum(centered * centered, axis=1, keepdims=True), "tp")
    spread = deviations / full_width
    return (centered * lax.rsqrt(spread + norm_eps) * out_gain).astype(jnp.bfloat16)


def shards(tokens, in_gain, expert_ids, route_weight, w_gate, w_up, w_down, out_gain):
    groups, parts = lax.axis_size("ep"), lax.axis_size("tp")
    tok_rows, width = tokens.shape
    local_experts = w_gate.shape[0]
    cap = capacity_of(tok_rows, expert_ids.shape[1], local_experts, local_experts * groups)
    whole_tiles = cap % 16 == 0 and (groups * cap) % 128 == 0 and width % (parts * 128) == 0
    if local_experts == 1 and parts % 2 == 0 and whole_tiles and groups * cap * width <= 1 << 20:
        return one_kernel(
            groups, parts, cap, tokens, in_gain, expert_ids.T, route_weight.T, w_gate, w_up, w_down, out_gain
        )
    return collectives(
        tokens, in_gain, expert_ids, route_weight, w_gate, w_up, w_down, out_gain
    )


def solution(mesh):
    in_specs = (
        P("ep", None),
        P(),
        P("ep", None),
        P("ep", None),
        P("ep", None, "tp"),
        P("ep", None, "tp"),
        P("ep", "tp", None),
        P("tp"),
    )
    out_specs = P("ep", "tp")
    return jax.shard_map(shards, mesh=mesh, in_specs=in_specs, out_specs=out_specs, check_vma=False)
```
